32 devices in a mesh: grp: 2 (over y), kv: 4 (over z), tp: 4 (over x, core).
Axes of the slice: x: 2, y: 2, z: 4, core: 2. Of those that a mesh axis runs over, the one named last changes fastest.
Arguments:
- tokens: bfloat16 [16, 4096], P('grp', 'kv'), parts along dimension 0, may hold values from -6 to 6
- norm_gain: float32 [4096], replicated, may hold values from 0.1 to 1.9
- w_query: bfloat16 [4096, 4096], P('kv', 'tp'), may hold values from -0.09375 to 0.09375
- key_weight: bfloat16 [4096, 512], P('kv', 'tp'), may hold values from -0.09375 to 0.09375
- value_weight: bfloat16 [4096, 512], P('kv', 'tp'), may hold values from -0.09375 to 0.09375
- w_gate: bfloat16 [4096, 64], replicated, may hold values from -0.09375 to 0.09375
- gate_bias: float32 [64], replicated, may hold values from -3 to 4
- w_out: bfloat16 [4096, 4096], P('kv', 'tp'), may hold values from -0.1875 to 0.1875
- cache_keys: bfloat16 [16, 3072, 512], P('grp', 'kv', 'tp'), parts along dimension 0, may hold values from -240 to 240
- cache_values: bfloat16 [16, 3072, 512], P('grp', 'kv', 'tp'), parts along dimension 0, may hold values from -8 to 8
- cache_gate: float32 [16, 64, 3072], P('grp', 'tp', 'kv'), parts along dimension 0, may hold values from -3072 to 0, as said below
- gate_total: float32 [16, 64], P('grp', 'tp'), parts along dimension 0, may hold values from -3072 to 0, as said below
- lengths: int32 [16], P('grp'), parts along dimension 0, may hold values from 1536 to 3072, as said below
Outputs:
- mixed: bfloat16 [16, 4096], P('grp', 'kv'), parts along dimension 0
- key_new: bfloat16 [16, 512], P('grp', 'tp'), parts along dimension 0
- value_new: bfloat16 [16, 512], P('grp', 'tp'), parts along dimension 0
The draws below stay inside these ranges and needn't reach their ends.
There are 2 independent parts, one for each index of `grp`. The reference program is written for one: setup_inputs(seed, part) draws one part's arguments, and reference() takes and returns one part's arrays. A program takes and returns all parts, laid end to end along the dimension named above; an argument that names none is the same for every part. Nothing has to cross between parts.
Inputs may be any that keep to these rules, and one draw needn't show every extreme that they name: `lengths`: one sequence of each draw has all 3072 positions cached. `cache_gate`: non-increasing along positions. `gate_total`: equal to cache_gate at position lengths - 1 of the same sequence and head.
All inputs are finite; a program needn't handle non-finite values.
Results may differ from the reference program's by a relative error of at most 0.015.
Values may be sent and summed in bfloat16 or wider, within the bound.
A program may use at most 64 MiB of HBM per device.

```python
import jax
import jax.numpy as jnp
from jax import lax

MODEL_WIDTH = 4096
QUERY_HEADS = 64
KEY_VALUE_HEADS = 8
HEAD_SIZE = 64
SEQUENCE_COUNT = 8
POSITIONS_SHARD = 768
CACHE_LENGTH = 3072
N_TP = 4


def gate_cumulative(key):
    array_shape = (SEQUENCE_COUNT, QUERY_HEADS, CACHE_LENGTH)
    slow_share = 0.5
    gradual = jax.random.bernoulli(jax.random.fold_in(key, 1), slow_share, (SEQUENCE_COUNT, QUERY_HEADS, 1)).astype(jnp.float32)
    slow_rate = jax.random.uniform(jax.random.fold_in(key, 2), (SEQUENCE_COUNT, QUERY_HEADS, 1), jnp.float32, 0.5, 2.0) / CACHE_LENGTH
    fast_rate = 1.0 / jax.random.uniform(jax.random.fold_in(key, 3), (SEQUENCE_COUNT, QUERY_HEADS, 1), jnp.float32, 30.0, 100.0)
    decay_rate = gradual * slow_rate + (1.0 - gradual) * fast_rate
    cache_blocks = CACHE_LENGTH // POSITIONS_SHARD
    multiplier = jnp.exp(jax.random.uniform(jax.random.fold_in(key, 4), (SEQUENCE_COUNT, QUERY_HEADS, cache_blocks, 1), jnp.float32, -0.7, 0.7))
    multiplier = jnp.broadcast_to(multiplier, (SEQUENCE_COUNT, QUERY_HEADS, cache_blocks, POSITIONS_SHARD)).reshape(array_shape)
    coarse_estimate = jax.random.uniform(jax.random.fold_in(key, 5), array_shape, jnp.float32, 0.5, 1.5)
    surge_enabled = jax.random.bernoulli(jax.random.fold_in(key, 6), 4.0 / CACHE_LENGTH, array_shape).astype(jnp.float32)
    surge_depth = jax.random.uniform(jax.random.fold_in(key, 7), array_shape, jnp.float32, 0.22, 0.69)
    logarithm_gates = -(decay_rate * multiplier * coarse_estimate) - surge_enabled * surge_depth * gradual
    return jnp.cumsum(logarithm_gates, axis=2)


def length_table(key):
    drawn = jax.random.randint(jax.random.fold_in(key, 21), (SEQUENCE_COUNT,), CACHE_LENGTH // 2, CACHE_LENGTH + 1).astype(jnp.int32)
    chosen = jax.random.randint(jax.random.fold_in(key, 22), (), 0, SEQUENCE_COUNT).astype(jnp.int32)
    return jnp.where(jnp.arange(SEQUENCE_COUNT, dtype=jnp.int32) == chosen, jnp.int32(CACHE_LENGTH), drawn).astype(jnp.int32)


def draw_lengths(key, part):
    return length_table(key)


def draw_cache_gate(key, part):
    return gate_cumulative(key)


def draw_gate_total(key, part):
    cumulative = gate_cumulative(key)
    last = (length_table(key) - 1).astype(jnp.int32)
    index = jnp.broadcast_to(last[:, None, None], (SEQUENCE_COUNT, QUERY_HEADS, 1))
    return jnp.take_along_axis(cumulative, index, axis=2)[:, :, 0]


def draw_cache_keys(key, part):
    array_shape = (SEQUENCE_COUNT, CACHE_LENGTH, KEY_VALUE_HEADS * HEAD_SIZE)
    base = jnp.clip(jax.random.normal(jax.random.fold_in(key, 31), array_shape, jnp.float32), -6.0, 6.0)
    return base.astype(jnp.bfloat16)


def draw_cache_values(key, part):
    array_shape = (SEQUENCE_COUNT, CACHE_LENGTH, KEY_VALUE_HEADS * HEAD_SIZE)
    cache_blocks = CACHE_LENGTH // POSITIONS_SHARD
    noise = jnp.clip(jax.random.normal(jax.random.fold_in(key, 41), array_shape, jnp.float32), -5.0, 5.0)
    position_shift = jnp.clip(jax.random.normal(jax.random.fold_in(key, 42), (SEQUENCE_COUNT, cache_blocks, 1, KEY_VALUE_HEADS * HEAD_SIZE), jnp.float32), -3.0, 3.0)
    position_shift = jnp.broadcast_to(position_shift, (SEQUENCE_COUNT, cache_blocks, POSITIONS_SHARD, KEY_VALUE_HEADS * HEAD_SIZE)).reshape(array_shape)
    return (noise + position_shift).astype(jnp.bfloat16)


def block_scale(key, shape, cuts, least, high):
    factor_of = 1.0
    for axis_at, blocks in cuts:
        steps = jax.random.uniform(jax.random.fold_in(jax.random.fold_in(key, 6), axis_at), (blocks,), jnp.float32, least / len(cuts), high / len(cuts))
        factor_of = factor_of * jnp.repeat(jnp.exp(steps), shape[axis_at] // blocks).reshape((-1,) + (1,) * (len(shape) - 1 - axis_at))
    return factor_of


def gaussian(rng, shape, deviation, most, pieces=(), kind=jnp.bfloat16):
    entries = deviation * jax.random.normal(rng, shape, jnp.float32)
    if pieces:
        entries = entries * block_scale(rng, shape, pieces, -0.22, 0.18)
    return jnp.clip(entries, -most, most).astype(kind)


def setup_inputs(seed: int = 0, part: int = 0) -> dict:
    streams_of = jax.random.split(jax.random.key(seed), 14)
    part_keys = jax.random.split(jax.random.fold_in(streams_of[13], part), 14)
    return {
        "tokens": gaussian(part_keys[0], (SEQUENCE_COUNT, MODEL_WIDTH), 1.0, 6.0, ((1, 4),)),
        "norm_gain": jnp.clip(1.0 + 0.18 * jax.random.normal(streams_of[1], (MODEL_WIDTH,), jnp.float32), 0.1, 1.9),
        "w_query": gaussian(streams_of[2], (MODEL_WIDTH, QUERY_HEADS * HEAD_SIZE), MODEL_WIDTH ** -0.5, 0.09375, ((0, 4), (1, 4))),
        "key_weight": gaussian(streams_of[3], (MODEL_WIDTH, KEY_VALUE_HEADS * HEAD_SIZE), MODEL_WIDTH ** -0.5, 0.09375, ((0, 4), (1, 4))),
        "value_weight": gaussian(streams_of[4], (MODEL_WIDTH, KEY_VALUE_HEADS * HEAD_SIZE), MODEL_WIDTH ** -0.5, 0.09375, ((0, 4), (1, 4))),
        "w_gate": gaussian(streams_of[5], (MODEL_WIDTH, QUERY_HEADS), MODEL_WIDTH ** -0.5, 0.09375),
        "gate_bias": jnp.clip(jax.random.uniform(streams_of[6], (QUERY_HEADS,), jnp.float32, -3.0, 4.0), -3.0, 4.0),
        "w_out": gaussian(streams_of[7], (MODEL_WIDTH, QUERY_HEADS * HEAD_SIZE), (QUERY_HEADS * HEAD_SIZE // 4) ** -0.5, 0.1875, ((0, 4), (1, 4))),
        "cache_keys": draw_cache_keys(jax.random.fold_in(jax.random.fold_in(streams_of[13], part), 71), part),
        "cache_values": draw_cache_values(jax.random.fold_in(jax.random.fold_in(streams_of[13], part), 71), part),
        "cache_gate": draw_cache_gate(jax.random.fold_in(jax.random.fold_in(streams_of[13], part), 71), part),
        "gate_total": draw_gate_total(jax.random.fold_in(jax.random.fold_in(streams_of[13], part), 71), part),
        "lengths": draw_lengths(jax.random.fold_in(jax.random.fold_in(streams_of[13], part), 71), part),
    }


NEG_FILL = -1e+30

def attend_one(items):
    query_vector, key_matrix, value_matrix, gate_matrix, tier_row, seq_length, key_current, value_current = items
    head_group = QUERY_HEADS // KEY_VALUE_HEADS
    logit_scale = HEAD_SIZE ** (-0.5)
    query_head_rows = query_vector.astype(jnp.float32).reshape(KEY_VALUE_HEADS, head_group, HEAD_SIZE)
    key_head_rows = key_matrix.astype(jnp.float32).reshape(CACHE_LENGTH, KEY_VALUE_HEADS, HEAD_SIZE)
    value_head_rows = value_matrix.astype(jnp.float32).reshape(CACHE_LENGTH, KEY_VALUE_HEADS, HEAD_SIZE)
    score_matrix = jnp.einsum('kgd,lkd->kgl', query_head_rows, key_head_rows) * logit_scale
    score_matrix = score_matrix + (tier_row[:, None] - gate_matrix).reshape(KEY_VALUE_HEADS, head_group, CACHE_LENGTH)
    valid = (jnp.arange(CACHE_LENGTH, dtype=jnp.int32) < seq_length)[None, None, :]
    score_matrix = jnp.where(valid, score_matrix, NEG_FILL)
    current_score = jnp.einsum('pcy,py->pc', query_head_rows, key_current.astype(jnp.float32).reshape(KEY_VALUE_HEADS, HEAD_SIZE)) * logit_scale
    top = jnp.maximum(lax.optimization_barrier(jnp.max(score_matrix, axis=-1)), current_score)
    weights = jnp.where(valid, jnp.exp(score_matrix - top[..., None]), 0.0)
    current_weight = jnp.exp(current_score - top)
    denominator = lax.optimization_barrier(jnp.sum(weights, axis=-1)) + current_weight
    rounded = lax.optimization_barrier(weights.astype(jnp.bfloat16)).astype(jnp.float32)
    total_sum = jnp.einsum('kgl,lkd->kgd', rounded, value_head_rows)
    total_sum = total_sum + current_weight[..., None] * value_current.astype(jnp.float32).reshape(KEY_VALUE_HEADS, 1, HEAD_SIZE)
    return (total_sum / denominator[..., None]).reshape(QUERY_HEADS * HEAD_SIZE).astype(jnp.bfloat16)

def reference(tokens, norm_gain, w_query, key_weight, value_weight, w_gate, gate_bias, w_out, cache_keys, cache_values, cache_gate, gate_total, lengths):
    features = tokens.astype(jnp.float32)
    normed = features * lax.rsqrt(lax.optimization_barrier(jnp.mean(features * features, axis=-1, keepdims=True)) + 1e-06) * norm_gain
    normed = normed.astype(jnp.bfloat16)
    query = jnp.dot(normed, w_query, preferred_element_type=jnp.float32).astype(jnp.bfloat16)
    key_new = jnp.dot(normed, key_weight, preferred_element_type=jnp.float32).astype(jnp.bfloat16)
    value_new = jnp.dot(normed, value_weight, preferred_element_type=jnp.float32).astype(jnp.bfloat16)
    log_gate = jax.nn.log_sigmoid(jnp.dot(normed, w_gate, preferred_element_type=jnp.float32) + gate_bias)
    level = gate_total + log_gate
    attended = lax.map(attend_one, (query, cache_keys, cache_values, cache_gate, level, lengths, key_new, value_new))
    width = QUERY_HEADS * HEAD_SIZE // N_TP
    groups = attended.astype(jnp.float32).reshape(SEQUENCE_COUNT, N_TP, width)
    out_rows = w_out.astype(jnp.float32).reshape(MODEL_WIDTH, N_TP, width)
    partial_value = jnp.einsum('stc,dtc->std', groups, out_rows)
    partial_value = lax.optimization_barrier(partial_value.astype(jnp.bfloat16)).astype(jnp.float32)
    mixed = lax.optimization_barrier(jnp.sum(partial_value, axis=1)).astype(jnp.bfloat16)
    return (mixed, key_new, value_new)
```

```python
import functools

import jax
import jax.numpy as jnp
from jax import lax
from jax.experimental import pallas as pl
from jax.experimental.pallas import tpu as pltpu
from jax.sharding import PartitionSpec as P

HEAD_SIZE = 64
NEG_FILL = -1e30
LANES = 128
SUBLANES = 8
UNROLL_PEERS = 8
QUERY_PIECES = 4
CACHE_PIECES = 4
NT = (((1,), (1,)), ((), ()))


def fold(count, body, carry):
    if count <= UNROLL_PEERS:
        for i in range(count):
            carry = body(i, carry)
        return carry
    return lax.fori_loop(0, count, body, carry)


def kernel(
    n_kv,
    n_tp,
    tokens_hbm,
    gain_hbm,
    query_hbm,
    key_hbm,
    value_hbm,
    gate_hbm,
    bias_hbm,
    out_hbm,
    keys_hbm,
    values_hbm,
    cgate_hbm,
    total_hbm,
    lengths_hbm,
    mixed_ref,
    knew_ref,
    vnew_ref,
    tokens_v,
    gain_v,
    query_v,
    key_v,
    value_v,
    gate_v,
    bias_v,
    out_v,
    keys_v,
    values_v,
    cgate_v,
    total_v,
    lengths_s,
    parts,
    blocks,
    stats,
    mixes,
    qrows,
    arows,
    square,
    loc,
    send1,
    recv1,
    send2,
    recv2,
    send3,
    recv3,
    send4,
    recv4,
):
    seqs, width = tokens_v.shape
    _, heads, positions = cgate_v.shape
    group = heads // 2
    qcols = query_v.shape[1]
    kcols = key_v.shape[1]
    all_heads = gate_v.shape[1]
    kv = lax.axis_index("kv")
    tp = lax.axis_index("tp")

    barrier = pltpu.get_barrier_semaphore()

    def greet(axis, me, n):
        def one(k, c):
            pl.semaphore_signal(
                barrier,
                inc=1,
                device_id={axis: lax.rem(me + 1 + k, n)},
                device_id_type=pl.DeviceIdType.MESH,
            )
            return c

        fold(n - 1, one, 0)

    greet("kv", kv, n_kv)
    greet("tp", tp, n_tp)

    slot = [0]

    def load(src, dst):
        copy = pltpu.make_async_copy(src, dst, loc.at[slot[0]])
        slot[0] += 1
        copy.start()
        return copy

    c_tokens = load(tokens_hbm, tokens_v)
    c_gain = load(gain_hbm, gain_v)
    rows = pl.ds(pl.multiple_of(kv * width, width), width)
    c_gate = load(gate_hbm.at[rows], gate_v)
    step = width // QUERY_PIECES
    c_query = [
        load(query_hbm.at[pl.ds(i * step, step)], query_v.at[pl.ds(i * step, step)])
        for i in range(QUERY_PIECES)
    ]
    c_key = load(key_hbm, key_v)
    c_value = load(value_hbm, value_v)
    c_bias = load(bias_hbm, bias_v)
    c_total = load(total_hbm, total_v)
    c_lengths = load(lengths_hbm, lengths_s)
    c_cgate = load(cgate_hbm, cgate_v)
    per = seqs // CACHE_PIECES
    c_keys = [
        load(keys_hbm.at[pl.ds(i * per, per)], keys_v.at[pl.ds(i * per, per)])
        for i in range(CACHE_PIECES)
    ]
    c_values = [
        load(values_hbm.at[pl.ds(i * per, per)], values_v.at[pl.ds(i * per, per)])
        for i in range(CACHE_PIECES)
    ]
    c_out = load(out_hbm, out_v)

    def exchange(axis, me, n, buf, send, recv):
        def one(k, c):
            pltpu.make_async_remote_copy(
                src_ref=buf.at[me],
                dst_ref=buf.at[me],
                send_sem=send.at[k],
                recv_sem=recv.at[me],
                device_id={axis: lax.rem(me + 1 + k, n)},
                device_id_type=pl.DeviceIdType.MESH,
            ).start()
            return c

        fold(n - 1, one, 0)

    def arrive(axis, me, n, buf, send, recv):
        def one(k, c):
            peer = lax.rem(me + 1 + k, n)
            copy = pltpu.make_async_remote_copy(
                src_ref=buf.at[me],
                dst_ref=buf.at[peer],
                send_sem=send.at[k],
                recv_sem=recv.at[peer],
                device_id={axis: peer},
                device_id_type=pl.DeviceIdType.MESH,
            )
            copy.wait()
            return c

        fold(n - 1, one, 0)

    lane = lax.broadcasted_iota(jnp.int32, (SUBLANES, LANES), 1)
    low = lane < HEAD_SIZE
    place = lane % HEAD_SIZE

    c_tokens.wait()
    c_gain.wait()
    x = tokens_v[...].astype(jnp.float32)
    squares = jnp.sum(x * x, axis=1, keepdims=True)
    if gain_v.shape[0] == 1:
        scaled = x * gain_v[...]
    else:
        chunks = width // LANES
        scaled = jnp.concatenate(
            [
                x[:, i * LANES : (i + 1) * LANES] * gain_v[pl.ds(kv * chunks + i, 1), :]
                for i in range(chunks)
            ],
            axis=1,
        )
    high = scaled.astype(jnp.bfloat16)
    rest = (scaled - high.astype(jnp.float32)).astype(jnp.bfloat16)
    both = jnp.concatenate([high, rest], axis=0)

    def project(weights, lhs=both):
        out = jnp.dot(lhs, weights, preferred_element_type=jnp.float32)
        return out[:seqs] + out[seqs:]

    c_gate.wait()
    gates = project(gate_v[...])
    base = qcols + 2 * kcols
    pair = jnp.concatenate(
        [gates, jnp.broadcast_to(squares, (seqs, LANES - all_heads))], axis=1
    )
    pair_high = pair.astype(jnp.bfloat16)
    parts[kv, :, base : base + LANES] = pair_high
    parts[kv, :, base + LANES : base + 2 * LANES] = (
        pair - pair_high.astype(jnp.float32)
    ).astype(jnp.bfloat16)
    acc = None
    for i in range(QUERY_PIECES):
        c_query[i].wait()
        cut = slice(i * step, (i + 1) * step)
        term = jnp.dot(both[:, cut], query_v[cut, :], preferred_element_type=jnp.float32)
        acc = term if acc is None else acc + term
    parts[kv, :, :qcols] = (acc[:seqs] + acc[seqs:]).astype(jnp.bfloat16)
    c_key.wait()
    parts[kv, :, qcols : qcols + kcols] = project(key_v[...]).astype(jnp.bfloat16)
    c_value.wait()
    parts[kv, :, qcols + kcols : base] = project(value_v[...]).astype(jnp.bfloat16)

    pl.semaphore_wait(barrier, n_kv - 1 + n_tp - 1)
    exchange("kv", kv, n_kv, parts, send1, recv1)

    c_total.wait()
    c_lengths.wait()
    c_cgate.wait()
    c_bias.wait()
    square[...] = jnp.zeros_like(square)
    square[:seqs, :heads] = total_v[...]
    total_t = jnp.transpose(square[...])[:heads, :]
    index = kv * positions + lax.broadcasted_iota(jnp.int32, (heads, positions), 1)
    for s in range(seqs):
        cgate_v[s] = jnp.where(
            index < lengths_s[s], total_t[:, s : s + 1] - cgate_v[s], NEG_FILL
        )

    arrive("kv", kv, n_kv, parts, send1, recv1)
    summed = fold(
        n_kv,
        lambda j, c: c + parts[j].astype(jnp.float32),
        jnp.zeros((seqs, base + 2 * LANES), jnp.float32),
    )
    pair = summed[:, base : base + LANES] + summed[:, base + LANES :]
    scale = lax.rsqrt(pair[:, all_heads : all_heads + 1] / (width * n_kv) + 1e-6)
    query = (summed[:, :qcols] * scale).astype(jnp.bfloat16).astype(jnp.float32)
    query = query * (HEAD_SIZE ** -0.5)
    knew = (summed[:, qcols : qcols + kcols] * scale).astype(jnp.bfloat16)
    vnew = (summed[:, qcols + kcols : base] * scale).astype(jnp.bfloat16)
    knew_ref[...] = knew
    vnew_ref[...] = vnew
    knew = knew.astype(jnp.float32)
    vnew = vnew.astype(jnp.float32)

    half = heads // 2
    for c in range(half):
        chunk = query[:, c * LANES : (c + 1) * LANES]
        turned = pltpu.roll(chunk, HEAD_SIZE, 1)
        if 2 * c < group:
            even, odd = jnp.where(low, chunk, 0.0), jnp.where(low, turned, 0.0)
        else:
            even, odd = jnp.where(low, 0.0, turned), jnp.where(low, 0.0, chunk)
        qrows[pl.ds(2 * c * seqs, seqs), :] = even
        qrows[pl.ds((2 * c + 1) * seqs, seqs), :] = odd

    def select(column):
        return jnp.where(low, column[:group], column[group:])

    stat = jnp.zeros((group, LANES), jnp.float32)
    held = None
    for s in range(seqs):
        if s % per == 0:
            c_keys[s // per].wait()
        q = qrows[pl.ds(s, heads, stride=seqs), :].astype(jnp.bfloat16)
        score = lax.dot_general(q, keys_v[s], NT, preferred_element_type=jnp.float32)
        score = score + cgate_v[s]
        peak = jnp.max(score, axis=1, keepdims=True)
        weight = jnp.exp(score - peak)
        mass = jnp.sum(weight, axis=1, keepdims=True)
        if s % per == 0:
            c_values[s // per].wait()
        value = jnp.dot(
            weight.astype(jnp.bfloat16), values_v[s], preferred_element_type=jnp.float32
        )
        stat = jnp.where(place == s, select(peak), stat)
        stat = jnp.where(place == seqs + s, select(mass), stat)
        mine = select(value)
        if s % 2 == 0:
            held = mine
        else:
            blocks[kv, (s - 1) * group : (s + 1) * group, :] = jnp.concatenate(
                [held, mine], axis=0
            ).astype(jnp.bfloat16)
    stats[kv] = stat
    exchange("kv", kv, n_kv, stats, send3, recv3)
    exchange("kv", kv, n_kv, blocks, send2, recv2)

    z = pair * scale
    z = z[:, :all_heads] + bias_v[...]
    z = jnp.minimum(z, 0.0) - jnp.log1p(jnp.exp(-jnp.abs(z)))
    square[:seqs, :all_heads] = z
    turned = pltpu.roll(square[:seqs, :], lax.rem(LANES - tp * heads, LANES), 1)
    square[:seqs, :] = turned
    z_t = jnp.transpose(square[...])
    log_gate = jnp.where(low, z_t[:group], pltpu.roll(z_t[group:heads], HEAD_SIZE, 1))
    own = jnp.zeros((group, LANES), jnp.float32)
    for s in range(seqs):
        q = qrows[pl.ds(s, heads, stride=seqs), :]
        own = jnp.where(
            place == s,
            select(jnp.sum(q * knew[s : s + 1, :], axis=1, keepdims=True)),
            own,
        )

    arrive("kv", kv, n_kv, stats, send3, recv3)
    peak = fold(
        n_kv - 1, lambda j, c: jnp.maximum(c, stats[j + 1]), stats[0]
    )
    top = jnp.maximum(peak + log_gate, own)
    own_weight = jnp.exp(own - top)

    def factor(j):
        return jnp.exp(stats[j] + (log_gate - top))

    shift = LANES - seqs
    denominator = fold(
        n_kv, lambda j, c: c + factor(j) * pltpu.roll(stats[j], shift, 1), own_weight
    )
    inverse = 1.0 / denominator

    def spread(a, s):
        return jnp.where(low, a[:, s : s + 1], a[:, HEAD_SIZE + s : HEAD_SIZE + s + 1])

    own_weight = own_weight * inverse
    sums = [spread(own_weight, s) * vnew[s : s + 1, :] for s in range(seqs)]
    arrive("kv", kv, n_kv, blocks, send2, recv2)

    def add(j, sums):
        a = factor(j) * inverse
        block = blocks[j].astype(jnp.float32)
        return [
            sums[s] + spread(a, s) * block[s * group : (s + 1) * group]
            for s in range(seqs)
        ]

    sums = fold(n_kv, add, sums)
    for s in range(seqs):
        arows[pl.ds(s * group, group), :] = sums[s]
    pieces = []
    for c in range(half):
        g = 2 * c % group
        first = arows[pl.ds(g, seqs, stride=group), :]
        second = arows[pl.ds(g + 1, seqs, stride=group), :]
        if 2 * c < group:
            pieces.append(jnp.where(low, first, pltpu.roll(second, HEAD_SIZE, 1)))
        else:
            pieces.append(jnp.where(low, pltpu.roll(first, HEAD_SIZE, 1), second))
    attended = jnp.concatenate(pieces, axis=1).astype(jnp.bfloat16)

    c_out.wait()
    mixes[tp] = lax.dot_general(
        attended, out_v[...], NT, preferred_element_type=jnp.float32
    ).astype(jnp.bfloat16)
    exchange("tp", tp, n_tp, mixes, send4, recv4)
    arrive("tp", tp, n_tp, mixes, send4, recv4)
    total = fold(
        n_tp,
        lambda j, c: c + mixes[j].astype(jnp.float32),
        jnp.zeros((seqs, width), jnp.float32),
    )
    mixed_ref[...] = total.astype(jnp.bfloat16)


def per_device(n_kv, n_tp, *args):
    (
        tokens,
        norm_gain,
        w_query,
        key_weight,
        value_weight,
        w_gate,
        gate_bias,
        w_out,
        cache_keys,
        cache_values,
        cache_gate,
        gate_total,
        lengths,
    ) = args
    seqs, width = tokens.shape
    _, heads, positions = cache_gate.shape
    qcols, kcols = w_query.shape[1], key_weight.shape[1]
    all_heads = w_gate.shape[1]
    if width % LANES == 0:
        gain = norm_gain.reshape(-1, LANES)
    else:
        start = lax.axis_index("kv") * width
        gain = lax.dynamic_slice_in_dim(norm_gain, start, width, 0).reshape(1, width)
    bias = gate_bias.reshape(1, all_heads)
    operands = (
        tokens,
        gain,
        w_query,
        key_weight,
        value_weight,
        w_gate,
        bias,
        w_out,
        cache_keys,
        cache_values,
        cache_gate,
        gate_total,
        lengths,
    )
    bf16, f32 = jnp.bfloat16, jnp.float32
    packed = qcols + 2 * kcols + 2 * LANES
    group = heads // 2
    n_loads = 10 + QUERY_PIECES + 2 * CACHE_PIECES
    dma = pltpu.SemaphoreType.DMA
    return pl.pallas_call(
        functools.partial(kernel, n_kv, n_tp),
        out_shape=(
            jax.ShapeDtypeStruct((seqs, width), bf16),
            jax.ShapeDtypeStruct((seqs, kcols), bf16),
            jax.ShapeDtypeStruct((seqs, kcols), bf16),
        ),
        in_specs=[pl.BlockSpec(memory_space=pl.ANY)] * len(operands),
        out_specs=(pl.BlockSpec(memory_space=pltpu.VMEM),) * 3,
        scratch_shapes=[
            pltpu.VMEM(tokens.shape, bf16),
            pltpu.VMEM(gain.shape, f32),
            pltpu.VMEM(w_query.shape, bf16),
            pltpu.VMEM(key_weight.shape, bf16),
            pltpu.VMEM(value_weight.shape, bf16),
            pltpu.VMEM((width, all_heads), bf16),
            pltpu.VMEM(bias.shape, f32),
            pltpu.VMEM(w_out.shape, bf16),
            pltpu.VMEM(cache_keys.shape, bf16),
            pltpu.VMEM(cache_values.shape, bf16),
            pltpu.VMEM(cache_gate.shape, f32),
            pltpu.VMEM(gate_total.shape, f32),
            pltpu.SMEM(lengths.shape, jnp.int32),
            pltpu.VMEM((n_kv, seqs, packed), bf16),
            pltpu.VMEM((n_kv, seqs * group, LANES), bf16),
            pltpu.VMEM((n_kv, group, LANES), f32),
            pltpu.VMEM((n_tp, seqs, width), bf16),
            pltpu.VMEM((heads * seqs, LANES), f32),
            pltpu.VMEM((seqs * group, LANES), f32),
            pltpu.VMEM((LANES, LANES), f32),
            dma((n_loads,)),
            dma((n_kv,)),
            dma((n_kv,)),
            dma((n_kv,)),
            dma((n_kv,)),
            dma((n_kv,)),
            dma((n_kv,)),
            dma((n_tp,)),
            dma((n_tp,)),
        ],
        compiler_params=pltpu.CompilerParams(
            collective_id=0, has_side_effects=True, vmem_limit_bytes=48 * 1024 * 1024
        ),
    )(*operands)


def solution(mesh):
    placed = (
        P("grp", "kv"),
        P(),
        P("kv", "tp"),
        P("kv", "tp"),
        P("kv", "tp"),
        P(),
        P(),
        P("kv", "tp"),
        P("grp", "kv", "tp"),
        P("grp", "kv", "tp"),
        P("grp", "tp", "kv"),
        P("grp", "tp"),
        P("grp"),
    )
    return jax.shard_map(
        functools.partial(per_device, mesh.shape["kv"], mesh.shape["tp"]),
        mesh=mesh,
        in_specs=placed,
        out_specs=(P("grp", "kv"), P("grp", "tp"), P("grp", "tp")),
        check_vma=False,
    )
```

```python
import functools

import jax
import jax.numpy as jnp
from jax import lax
from jax.experimental import pallas as pl
from jax.experimental.pallas import tpu as pltpu
from jax.sharding import PartitionSpec as P

HEAD_SIZE = 64
NEG_FILL = -1e30
LANES = 128
SUBLANES = 8
UNROLL_PEERS = 8
QUERY_PIECES = 2
CACHE_PIECES = 4
BLOCK_PIECES = 1
OUT_PIECES = 1
NT = (((1,), (1,)), ((), ()))


def fold(count, body, carry):
    if count <= UNROLL_PEERS:
        for i in range(count):
            carry = body(i, carry)
        return carry
    return lax.fori_loop(0, count, body, carry)


def kernel(
    n_kv,
    n_tp,
    tokens_hbm,
    gain_hbm,
    query_hbm,
    key_hbm,
    value_hbm,
    gate_hbm,
    bias_hbm,
    out_hbm,
    keys_hbm,
    values_hbm,
    cgate_hbm,
    total_hbm,
    lengths_hbm,
    packed_ref,
    tokens_v,
    gain_v,
    query_v,
    key_v,
    value_v,
    gate_v,
    bias_v,
    out_v,
    keys_v,
    values_v,
    cgate_v,
    total_v,
    lengths_s,
    parts,
    blocks,
    stats,
    mixes,
    qrows,
    arows,
    square,
    loc,
    send1,
    recv1,
    send2,
    recv2,
    send4,
    recv4,
):
    sems1, sems2, sems4 = (
        (send1, recv1),
        (send2, recv2),
        (send4, recv4),
    )
    seqs, width = tokens_v.shape
    _, heads, positions = cgate_v.shape
    group = heads // 2
    qcols = query_v.shape[1]
    kcols = key_v.shape[1]
    all_heads = gate_v.shape[0]
    kv = lax.axis_index("kv")
    tp = lax.axis_index("tp")

    barrier = pltpu.get_barrier_semaphore()

    def greet(axis, me, n):
        def one(k, c):
            pl.semaphore_signal(
                barrier,
                inc=1,
                device_id={axis: lax.rem(me + 1 + k, n)},
                device_id_type=pl.DeviceIdType.MESH,
            )
            return c

        fold(n - 1, one, 0)

    greet("kv", kv, n_kv)
    greet("tp", tp, n_tp)

    def span(start, size):
        return (slice(None), pl.ds(start, size))

    slot = [0]

    def load(src, dst):
        copy = pltpu.make_async_copy(src, dst, loc.at[slot[0]])
        slot[0] += 1
        copy.start()
        return copy

    c_tokens = load(tokens_hbm, tokens_v)
    c_gain = load(gain_hbm, gain_v)
    c_gate = load(gate_hbm if gate_hbm.shape == gate_v.shape else gate_hbm.at[:, pl.ds(pl.multiple_of(kv * width, width), width)], gate_v)
    c_key = load(key_hbm, key_v)
    c_value = load(value_hbm, value_v)
    step = qcols // QUERY_PIECES
    c_query = [
        load(query_hbm.at[span(i * step, step)], query_v.at[span(i * step, step)])
        for i in range(QUERY_PIECES)
    ]
    c_bias = load(bias_hbm, bias_v)
    c_total = load(total_hbm, total_v)
    c_lengths = load(lengths_hbm, lengths_s)
    c_cgate = load(cgate_hbm, cgate_v)
    per = seqs // CACHE_PIECES
    c_keys = [
        load(keys_hbm.at[pl.ds(i * per, per)], keys_v.at[pl.ds(i * per, per)])
        for i in range(CACHE_PIECES)
    ]
    c_values = [
        load(values_hbm.at[pl.ds(i * per, per)], values_v.at[pl.ds(i * per, per)])
        for i in range(CACHE_PIECES)
    ]
    out_pieces = sems4[0].shape[0]
    depth = width // out_pieces
    c_out = [
        load(out_hbm.at[pl.ds(i * depth, depth)], out_v.at[pl.ds(i * depth, depth)])
        for i in range(out_pieces)
    ]

    def remote(axis, me, n, buf, sems, piece, cut, k, slot):
        send, recv = sems
        return pltpu.make_async_remote_copy(
            src_ref=buf.at[me, *cut] if cut else buf.at[me],
            dst_ref=buf.at[slot, *cut] if cut else buf.at[slot],
            send_sem=send.at[piece, k],
            recv_sem=recv.at[piece, slot],
            device_id={axis: lax.rem(me + 1 + k, n)},
            device_id_type=pl.DeviceIdType.MESH,
        )

    def exchange(axis, me, n, buf, sems, piece=0, cut=()):
        def one(k, c):
            remote(axis, me, n, buf, sems, piece, cut, k, me).start()
            return c

        fold(n - 1, one, 0)

    def arrive(axis, me, n, buf, sems, piece=0, cut=()):
        def one(k, c):
            slot = lax.rem(me + 1 + k, n)
            remote(axis, me, n, buf, sems, piece, cut, k, slot).wait()
            return c

        fold(n - 1, one, 0)

    lane = lax.broadcasted_iota(jnp.int32, (SUBLANES, LANES), 1)
    low = lane < HEAD_SIZE
    place = lane % HEAD_SIZE

    c_tokens.wait()
    c_gain.wait()
    x = tokens_v[...].astype(jnp.float32)
    squares = jnp.sum(x * x, axis=1, keepdims=True)
    if gain_v.shape[0] == 1:
        scaled = x * gain_v[...]
    else:
        chunks = width // LANES
        scaled = jnp.concatenate(
            [
                x[:, i * LANES : (i + 1) * LANES] * gain_v[pl.ds(kv * chunks + i, 1), :]
                for i in range(chunks)
            ],
            axis=1,
        )
    high = scaled.astype(jnp.bfloat16)
    rest = (scaled - high.astype(jnp.float32)).astype(jnp.bfloat16)
    both = jnp.concatenate([high, rest], axis=0)

    def project(weights, lhs=both):
        out = jnp.dot(lhs, weights, preferred_element_type=jnp.float32)
        return out[:seqs] + out[seqs:]

    c_gate.wait()
    gates = lax.dot_general(both, gate_v[...], NT, preferred_element_type=jnp.float32)
    gates = gates[:seqs] + gates[seqs:]
    base = 2 * kcols
    side = base + 2 * LANES
    pair = jnp.concatenate(
        [gates, jnp.broadcast_to(squares, (seqs, LANES - all_heads))], axis=1
    )
    pair_high = pair.astype(jnp.bfloat16)
    parts[kv, :, base : base + LANES] = pair_high
    parts[kv, :, base + LANES : side] = (pair - pair_high.astype(jnp.float32)).astype(
        jnp.bfloat16
    )
    c_key.wait()
    parts[kv, :, :kcols] = project(key_v[...]).astype(jnp.bfloat16)
    c_value.wait()
    parts[kv, :, kcols:base] = project(value_v[...]).astype(jnp.bfloat16)
    for i in range(QUERY_PIECES):
        c_query[i].wait()
        parts[kv, :, side + i * step : side + (i + 1) * step] = project(
            query_v[:, i * step : (i + 1) * step]
        ).astype(jnp.bfloat16)
    pl.semaphore_wait(barrier, n_kv - 1 + n_tp - 1)
    exchange("kv", kv, n_kv, parts, sems1)

    c_total.wait()
    c_lengths.wait()
    c_cgate.wait()
    c_bias.wait()
    square[...] = jnp.zeros_like(square)
    square[:seqs, :heads] = total_v[...]
    total_t = jnp.transpose(square[...])[:heads, :]
    index = kv * positions + lax.broadcasted_iota(jnp.int32, (heads, positions), 1)
    for s in range(seqs):
        cgate_v[s] = jnp.where(
            index < lengths_s[s], total_t[:, s : s + 1] - cgate_v[s], NEG_FILL
        )

    arrive("kv", kv, n_kv, parts, sems1)
    summed = fold(
        n_kv,
        lambda j, c: c + parts[j].astype(jnp.float32),
        jnp.zeros((seqs, side + qcols), jnp.float32),
    )
    pair = summed[:, base : base + LANES] + summed[:, base + LANES : side]
    scale = lax.rsqrt(pair[:, all_heads : all_heads + 1] / (width * n_kv) + 1e-6)
    query = (summed[:, side:] * scale).astype(jnp.bfloat16).astype(jnp.float32)
    query = query * (HEAD_SIZE ** -0.5)
    knew = (summed[:, :kcols] * scale).astype(jnp.bfloat16)
    vnew = (summed[:, kcols:base] * scale).astype(jnp.bfloat16)
    packed_ref[:, :kcols] = knew
    packed_ref[:, kcols : 2 * kcols] = vnew
    knew = knew.astype(jnp.float32)
    vnew = vnew.astype(jnp.float32)

    half = heads // 2
    for c in range(half):
        chunk = query[:, c * LANES : (c + 1) * LANES]
        turned = pltpu.roll(chunk, HEAD_SIZE, 1)
        if 2 * c < group:
            even, odd = jnp.where(low, chunk, 0.0), jnp.where(low, turned, 0.0)
        else:
            even, odd = jnp.where(low, 0.0, turned), jnp.where(low, 0.0, chunk)
        qrows[pl.ds(2 * c * seqs, seqs), :] = even
        qrows[pl.ds((2 * c + 1) * seqs, seqs), :] = odd

    def select(column):
        return jnp.where(low, column[:group], column[group:])

    for copy in c_keys + c_values:
        copy.wait()
    stat = jnp.zeros((group, LANES), jnp.float32)
    held = None
    share = seqs // BLOCK_PIECES
    for s in range(seqs):
        q = qrows[pl.ds(s, heads, stride=seqs), :].astype(jnp.bfloat16)
        score = lax.dot_general(q, keys_v[s], NT, preferred_element_type=jnp.float32)
        score = score + cgate_v[s]
        peak = jnp.max(score, axis=1, keepdims=True)
        weight = jnp.exp(score - peak)
        mass = jnp.sum(weight, axis=1, keepdims=True)
        value = jnp.dot(
            weight.astype(jnp.bfloat16), values_v[s], preferred_element_type=jnp.float32
        )
        stat = jnp.where(place == s, select(peak), stat)
        stat = jnp.where(place == seqs + s, select(mass), stat)
        mine = select(value)
        if s % 2 == 0:
            held = mine
        else:
            blocks[kv, (s - 1) * group : (s + 1) * group, :] = jnp.concatenate(
                [held, mine], axis=0
            ).astype(jnp.bfloat16)
        if s == seqs - 1:
            left = stat
            for i in range(2):
                digits = []
                for _ in range(2):
                    digit = left.astype(jnp.bfloat16)
                    left = left - digit.astype(jnp.float32)
                    digits.append(digit)
                first = seqs * group + 2 * i * group
                blocks[kv, first : first + 2 * group, :] = jnp.concatenate(digits, axis=0)
        if (s + 1) % share == 0:
            exchange("kv", kv, n_kv, blocks, sems2)

    z = pair * scale
    z = z[:, :all_heads] + bias_v[...]
    z = jnp.minimum(z, 0.0) - jnp.log1p(jnp.exp(-jnp.abs(z)))
    square[:seqs, :all_heads] = z
    turned = pltpu.roll(square[:seqs, :], lax.rem(LANES - tp * heads, LANES), 1)
    square[:seqs, :] = turned
    z_t = jnp.transpose(square[...])
    log_gate = jnp.where(low, z_t[:group], pltpu.roll(z_t[group:heads], HEAD_SIZE, 1))
    own = jnp.zeros((group, LANES), jnp.float32)
    for s in range(seqs):
        q = qrows[pl.ds(s, heads, stride=seqs), :]
        own = jnp.where(
            place == s,
            select(jnp.sum(q * knew[s : s + 1, :], axis=1, keepdims=True)),
            own,
        )

    arrive("kv", kv, n_kv, blocks, sems2)

    def gather(j, c):
        digits = blocks[j, seqs * group :, :].astype(jnp.float32)
        total = digits[:group]
        for i in range(1, 4):
            total = total + digits[i * group : (i + 1) * group]
        stats[j] = total
        return c

    fold(n_kv, gather, 0)
    peak = fold(
        n_kv - 1, lambda j, c: jnp.maximum(c, stats[j + 1]), stats[0]
    )
    top = jnp.maximum(peak + log_gate, own)
    own_weight = jnp.exp(own - top)

    def factor(j):
        return jnp.exp(stats[j] + (log_gate - top))

    shift = LANES - seqs
    denominator = fold(
        n_kv, lambda j, c: c + factor(j) * pltpu.roll(stats[j], shift, 1), own_weight
    )
    inverse = 1.0 / denominator

    def spread(a, s):
        return jnp.where(low, a[:, s : s + 1], a[:, HEAD_SIZE + s : HEAD_SIZE + s + 1])

    own_weight = own_weight * inverse
    sums = [spread(own_weight, s) * vnew[s : s + 1, :] for s in range(seqs)]

    def add(j, sums):
        a = factor(j) * inverse
        block = blocks[j, : seqs * group, :].astype(jnp.float32)
        return [
            sums[s] + spread(a, s) * block[s * group : (s + 1) * group]
            for s in range(seqs)
        ]

    sums = fold(n_kv, add, sums)
    for s in range(seqs):
        arows[pl.ds(s * group, group), :] = sums[s]
    pieces = []
    for c in range(half):
        g = 2 * c % group
        first = arows[pl.ds(g, seqs, stride=group), :]
        second = arows[pl.ds(g + 1, seqs, stride=group), :]
        if 2 * c < group:
            pieces.append(jnp.where(low, first, pltpu.roll(second, HEAD_SIZE, 1)))
        else:
            pieces.append(jnp.where(low, pltpu.roll(first, HEAD_SIZE, 1), second))
    attended = jnp.concatenate(pieces, axis=1).astype(jnp.bfloat16)

    for i in range(out_pieces):
        c_out[i].wait()
        mixes[tp, :, i * depth : (i + 1) * depth] = lax.dot_general(
            attended,
            out_v[i * depth : (i + 1) * depth, :],
            NT,
            preferred_element_type=jnp.float32,
        ).astype(jnp.bfloat16)
        exchange("tp", tp, n_tp, mixes, sems4, i, span(i * depth, depth))
    for i in range(out_pieces):
        arrive("tp", tp, n_tp, mixes, sems4, i, span(i * depth, depth))
    total = fold(
        n_tp,
        lambda j, c: c + mixes[j].astype(jnp.float32),
        jnp.zeros((seqs, width), jnp.float32),
    )
    packed_ref[:, 2 * kcols :] = total.astype(jnp.bfloat16)


def unpack(packed_ref, mixed_ref, knew_ref, vnew_ref):
    kcols = knew_ref.shape[1]
    knew_ref[...] = packed_ref[:, :kcols]
    vnew_ref[...] = packed_ref[:, kcols : 2 * kcols]
    mixed_ref[...] = packed_ref[:, 2 * kcols :]


def per_device(n_kv, n_tp, *args):
    (
        tokens,
        norm_gain,
        w_query,
        key_weight,
        value_weight,
        w_gate,
        gate_bias,
        w_out,
        cache_keys,
        cache_values,
        cache_gate,
        gate_total,
        lengths,
    ) = args
    seqs, width = tokens.shape
    _, heads, positions = cache_gate.shape
    qcols, kcols = w_query.shape[1], key_weight.shape[1]
    all_heads = w_gate.shape[1]
    gate = w_gate.T
    if width % LANES == 0:
        gain = norm_gain.reshape(-1, LANES)
    else:
        start = lax.axis_index("kv") * width
        gate = lax.dynamic_slice_in_dim(gate, start, width, 1)
        gain = lax.dynamic_slice_in_dim(norm_gain, start, width, 0).reshape(1, width)
    bias = gate_bias.reshape(1, all_heads)
    operands = (
        tokens,
        gain,
        w_query,
        key_weight,
        value_weight,
        gate,
        bias,
        w_out,
        cache_keys,
        cache_values,
        cache_gate,
        gate_total,
        lengths,
    )
    bf16, f32 = jnp.bfloat16, jnp.float32
    packed = qcols + 2 * kcols + 2 * LANES
    group = heads // 2
    out_pieces = OUT_PIECES if width % (OUT_PIECES * LANES) == 0 else 1
    n_loads = 9 + QUERY_PIECES + 2 * CACHE_PIECES + out_pieces
    dma = pltpu.SemaphoreType.DMA
    results = pl.pallas_call(
        functools.partial(kernel, n_kv, n_tp),
        out_shape=pltpu.VMEM((seqs, width + 2 * kcols), bf16),
        in_specs=[pl.BlockSpec(memory_space=pltpu.HBM)] * len(operands),
        out_specs=pl.BlockSpec(memory_space=pltpu.VMEM),
        scratch_shapes=[
            pltpu.VMEM(tokens.shape, bf16),
            pltpu.VMEM(gain.shape, f32),
            pltpu.VMEM(w_query.shape, bf16),
            pltpu.VMEM(key_weight.shape, bf16),
            pltpu.VMEM(value_weight.shape, bf16),
            pltpu.VMEM((all_heads, width), bf16),
            pltpu.VMEM(bias.shape, f32),
            pltpu.VMEM(w_out.shape, bf16),
            pltpu.VMEM(cache_keys.shape, bf16),
            pltpu.VMEM(cache_values.shape, bf16),
            pltpu.VMEM(cache_gate.shape, f32),
            pltpu.VMEM(gate_total.shape, f32),
            pltpu.SMEM(lengths.shape, jnp.int32),
            pltpu.VMEM((n_kv, seqs, packed), bf16),
            pltpu.VMEM((n_kv, (seqs + 4) * group, LANES), bf16),
            pltpu.VMEM((n_kv, group, LANES), f32),
            pltpu.VMEM((n_tp, seqs, width), bf16),
            pltpu.VMEM((heads * seqs, LANES), f32),
            pltpu.VMEM((seqs * group, LANES), f32),
            pltpu.VMEM((LANES, LANES), f32),
            dma((n_loads,)),
            dma((1, n_kv)),
            dma((1, n_kv)),
            dma((BLOCK_PIECES, n_kv)),
            dma((BLOCK_PIECES, n_kv)),
            dma((out_pieces, n_tp)),
            dma((out_pieces, n_tp)),
        ],
        compiler_params=pltpu.CompilerParams(
            collective_id=0, has_side_effects=True, vmem_limit_bytes=67043328 - 64 * 1024
        ),
    )(*operands)
    vmem = pl.BlockSpec(memory_space=pltpu.VMEM)
    return pl.pallas_call(
        unpack,
        out_shape=(
            jax.ShapeDtypeStruct((seqs, width), bf16),
            jax.ShapeDtypeStruct((seqs, kcols), bf16),
            jax.ShapeDtypeStruct((seqs, kcols), bf16),
        ),
        in_specs=[vmem],
        out_specs=(vmem,) * 3,
        compiler_params=pltpu.CompilerParams(vmem_limit_bytes=2 * 1024 * 1024),
    )(results)


def solution(mesh):
    placed = (
        P("grp", "kv"),
        P(),
        P("kv", "tp"),
        P("kv", "tp"),
        P("kv", "tp"),
        P(),
        P(),
        P("kv", "tp"),
        P("grp", "kv", "tp"),
        P("grp", "kv", "tp"),
        P("grp", "tp", "kv"),
        P("grp", "tp"),
        P("grp"),
    )
    return jax.shard_map(
        functools.partial(per_device, mesh.shape["kv"], mesh.shape["tp"]),
        mesh=mesh,
        in_specs=placed,
        out_specs=(P("grp", "kv"), P("grp", "tp"), P("grp", "tp")),
        check_vma=False,
    )
```
